32 devices in a mesh: sp: 8 (over z, x), tp: 4 (over y, core).
Axes of the slice: x: 2, y: 2, z: 4, core: 2. Of those that a mesh axis runs over, the one named last changes fastest.
Arguments:
- conv_gate: bfloat16 [2048, 512], P('sp', 'tp'), may hold values from -6 to 6
- conv_mix: bfloat16 [2048, 512], P('sp', 'tp'), may hold values from -6 to 6
- conv_input: bfloat16 [2048, 512], P('sp', 'tp'), may hold values from -6 to 6
- conv_taps: bfloat16 [3, 512], P(None, 'tp'), may hold values from -3.5 to 3.5
- query_rows: bfloat16 [2048, 512], P('sp', 'tp'), may hold values from -50 to 50, as said below
- key_rows: bfloat16 [2048, 512], P('sp', 'tp'), may hold values from -10 to 10, as said below
- value_rows: bfloat16 [2048, 512], P('sp', 'tp'), may hold values from -6 to 6
- lambdas: float32 [4], P('tp'), may hold values from 0.3 to 0.8
- head_gain: float32 [128], replicated, may hold values from 0.1 to 1.9
- w_out_conv: bfloat16 [512, 2048], P('tp'), may hold values from -0.1875 to 0.1875
- w_out_heads: bfloat16 [512, 2048], P('tp'), may hold values from -0.1875 to 0.1875
Outputs:
- mixed: bfloat16 [2048, 2048], P(('sp', 'tp'))
The draws below stay inside these ranges and needn't reach their ends.
Inputs may be any that keep to these rules, and one draw needn't show every extreme that they name: `query_rows`: queries of order one; some rows may be far larger. `key_rows`: keys of order one.
All inputs are finite; a program needn't handle non-finite values.
Results may differ from the reference program's by a relative error of at most 0.013.
Values may be sent and summed in bfloat16 or wider, within the bound.
A program may use at most 128 MiB of HBM per device.

```python
import math
import jax
import jax.numpy as jnp
from jax import lax

D = 2048
CONV = 512
QHEADS = 4
KVHEADS = 4
HEAD_QK = 64
HEAD_V = 128
TAPS = 3
TOKENS = 2048
N_TP = 4


def drawn_pair(key):
    base_key = jax.random.fold_in(key, 7)
    key_draw = jax.random.fold_in(base_key, 1)
    query_draw = jax.random.fold_in(base_key, 2)
    key_vals = jnp.clip(1.3 * jax.random.normal(key_draw, (TOKENS, KVHEADS, 2, HEAD_QK), jnp.float32), -8.0, 8.0)
    query_vals = jnp.clip(1.3 * jax.random.normal(query_draw, (TOKENS, QHEADS, 2, HEAD_QK), jnp.float32), -8.0, 8.0)
    return (query_vals.reshape(TOKENS, QHEADS * 2 * HEAD_QK), key_vals.reshape(TOKENS, KVHEADS * 2 * HEAD_QK))


def draw_query_rows(key, part):
    return drawn_pair(key)[0].astype(jnp.bfloat16)


def draw_key_rows(key, part):
    return drawn_pair(key)[1].astype(jnp.bfloat16)


def block_levels(own_key, dims, shards, least, high):
    factor_of, own = 1.0, jax.random.fold_in(own_key, 6)
    for position, shards_of in shards:
        draws = jnp.exp(jax.random.uniform(jax.random.fold_in(own, position), (shards_of,), jnp.float32, least / len(shards), high / len(shards)))
        factor_of = factor_of * jnp.repeat(draws, dims[position] // shards_of).reshape([-1 if axis == position else 1 for axis in range(len(dims))])
    return factor_of


def centred(rng, extent, scale, limit, shards=(), kind=jnp.bfloat16):
    entries = jax.random.normal(rng, extent, jnp.float32) * scale
    if len(shards) > 0:
        entries = block_levels(rng, extent, shards, -0.22, 0.18) * entries
    return jnp.clip(entries, min=-limit, max=limit).astype(kind)


def setup_inputs(seed: int = 0) -> dict:
    seeds = jax.random.split(jax.random.key(seed), 12)
    conv_gate = centred(seeds[0], (TOKENS, CONV), 1.0, 6.0, ((0, 8), (1, 4)))
    conv_mix = centred(seeds[1], (TOKENS, CONV), 1.0, 6.0, ((0, 8), (1, 4)))
    conv_input = centred(seeds[2], (TOKENS, CONV), 1.0, 6.0, ((0, 8), (1, 4)))
    conv_taps = centred(seeds[3], (TAPS, CONV), TAPS ** -0.5, 3.5, ((1, 4),))
    query_rows = draw_query_rows(jax.random.fold_in(seeds[11], 71), 0)
    key_rows = draw_key_rows(jax.random.fold_in(seeds[11], 71), 0)
    value_rows = centred(seeds[6], (TOKENS, KVHEADS * HEAD_V), 1.0, 6.0, ((0, 8), (1, 4)))
    lambdas = jnp.clip(0.3 + 0.5 * jax.random.uniform(seeds[7], (QHEADS,), jnp.float32) ** block_levels(seeds[7], (QHEADS,), ((0, 4),), -0.2, 0.2), 0.3, 0.8)
    head_gain = jnp.clip(1.0 + 0.18 * jax.random.normal(seeds[8], (HEAD_V,), jnp.float32), 0.1, 1.9)
    w_out_conv = centred(seeds[9], (CONV, D), (CONV + QHEADS * HEAD_V) ** -0.5, 0.1875, ((0, 4),))
    w_out_heads = centred(seeds[10], (QHEADS * HEAD_V, D), (CONV + QHEADS * HEAD_V) ** -0.5, 0.1875, ((0, 4),))
    return {"conv_gate": conv_gate, "conv_mix": conv_mix, "conv_input": conv_input, "conv_taps": conv_taps, "query_rows": query_rows, "key_rows": key_rows, "value_rows": value_rows, "lambdas": lambdas, "head_gain": head_gain, "w_out_conv": w_out_conv, "w_out_heads": w_out_heads}


def conv_branch(conv_gate, conv_mix, conv_input, conv_taps):
    gated_in = (conv_mix.astype(jnp.float32) * conv_input.astype(jnp.float32)).astype(jnp.bfloat16)
    padded = jnp.pad(gated_in, ((2, 0), (0, 0))).astype(jnp.float32)
    tap_values = conv_taps.astype(jnp.float32)
    convolved = tap_values[0] * padded[:-2] + tap_values[1] * padded[1:-1] + tap_values[2] * padded[2:]
    return (conv_gate.astype(jnp.float32) * convolved).astype(jnp.bfloat16)

def attention(query_rows, key_rows, value_rows, lambdas, head_gain):
    tokens = query_rows.shape[0]
    qblock = math.gcd(tokens, 256)
    group_size = QHEADS // KVHEADS
    scale_qk = HEAD_QK ** (-0.5)
    query_heads = query_rows.reshape(tokens, QHEADS, 2, HEAD_QK).astype(jnp.float32)
    key_heads = key_rows.reshape(tokens, KVHEADS, 2, HEAD_QK).astype(jnp.float32)
    value_heads = value_rows.reshape(tokens, KVHEADS, HEAD_V).astype(jnp.float32)
    key_positions = jnp.arange(tokens, dtype=jnp.int32)

    def one_block(block_index):
        offset_at = block_index * qblock
        query_block = lax.dynamic_slice_in_dim(query_heads, offset_at, qblock, 0)
        allowed = key_positions[None, :] <= (offset_at + jnp.arange(qblock, dtype=jnp.int32))[:, None]
        pieces = []
        for kv_head in range(KVHEADS):
            query_group = query_block[:, kv_head * group_size:(kv_head + 1) * group_size]
            scores = jnp.einsum('bhmd,tmd->hmbt', query_group, key_heads[:, kv_head]) * scale_qk
            scores = jnp.where(allowed, scores, -jnp.inf)
            peak_val = lax.optimization_barrier(jnp.max(scores, axis=-1, keepdims=True))
            weights = jnp.exp(scores - peak_val)
            denoms = lax.optimization_barrier(jnp.sum(weights, axis=-1))
            rounded = lax.optimization_barrier(weights.astype(jnp.bfloat16)).astype(jnp.float32)
            numerator = jnp.einsum('hmbt,te->hmbe', rounded, value_heads[:, kv_head])
            lambda_col = lambdas[kv_head * group_size:(kv_head + 1) * group_size][:, None, None]
            pieces.append(numerator[:, 0] / denoms[:, 0, :, None] - lambda_col * numerator[:, 1] / denoms[:, 1, :, None])
        merged = jnp.concatenate(pieces, axis=0)
        merged = merged * lax.rsqrt(lax.optimization_barrier(jnp.mean(merged * merged, axis=-1, keepdims=True)) + 1e-06) * head_gain * 0.8
        return jnp.transpose(merged, (1, 0, 2)).reshape(qblock, QHEADS * HEAD_V).astype(jnp.bfloat16)
    blocks_out = lax.map(one_block, jnp.arange(tokens // qblock, dtype=jnp.int32))
    return blocks_out.reshape(tokens, QHEADS * HEAD_V)

def reference(conv_gate, conv_mix, conv_input, conv_taps, query_rows, key_rows, value_rows, lambdas, head_gain, w_out_conv, w_out_heads):
    conv_out = conv_branch(conv_gate, conv_mix, conv_input, conv_taps)
    head_out = attention(query_rows, key_rows, value_rows, lambdas, head_gain)
    conv_width = CONV // N_TP
    head_width = QHEADS * HEAD_V // N_TP
    summed = jnp.zeros((conv_out.shape[0], D), jnp.float32)
    for group_index in range(N_TP):
        conv_part = jnp.dot(conv_out[:, group_index * conv_width:(group_index + 1) * conv_width], w_out_conv[group_index * conv_width:(group_index + 1) * conv_width], preferred_element_type=jnp.float32)
        head_part = jnp.dot(head_out[:, group_index * head_width:(group_index + 1) * head_width], w_out_heads[group_index * head_width:(group_index + 1) * head_width], preferred_element_type=jnp.float32)
        partial_value = (conv_part + head_part).astype(jnp.bfloat16)
        summed = summed + partial_value.astype(jnp.float32)
    return summed.astype(jnp.bfloat16)
```

```python
import functools

import jax
import jax.numpy as jnp
from jax import lax
from jax.experimental import pallas as pl
from jax.experimental.pallas import tpu as pltpu
from jax.sharding import PartitionSpec as P

HEAD_QK = 64
PIECES = 2
COL_TILE = 512
LATE_TILES = 1
MESH = pl.DeviceIdType.MESH
F32 = jnp.float32
BF16 = jnp.bfloat16


def kernel(
    n_sp,
    n_tp,
    gate_h,
    mix_h,
    inp_h,
    taps_h,
    q_h,
    k_h,
    v_h,
    lam_ref,
    gain_h,
    wc_h,
    wh_h,
    out_ref,
    gate,
    mix,
    inp,
    taps,
    gain,
    q,
    col,
    cross,
    halo,
    ext,
    conv,
    wc,
    wh,
    cxs,
    cxr,
    cys,
    cyr,
    own,
    fxs,
    fxr,
    head,
    hact,
    pys,
    pyr,
    peak,
    denom,
    acc,
    load_sem,
    halo_ss,
    halo_rs,
    up_ss,
    col_rs,
    x_ss,
    cross_rs,
    w_ss,
    w_rs,
    cx_ss,
    cx_rs,
    cy_ss,
    cy_rs,
    ha_ss,
    ha_rs,
    fx_ss,
    fx_rs,
    py_ss,
    py_rs,
):
    s = lax.axis_index("sp")
    t = lax.axis_index("tp")
    levels, outer = n_sp // 2, n_tp // 2
    z, x = s // 2, s % 2
    a, b = t // 2, t % 2
    rows = q.shape[0]
    width = out_ref.shape[1]
    chunk = rows // n_tp
    piece = rows // PIECES
    has_next = s < n_sp - 1
    has_prev = s > 0
    has_up = z < levels - 1
    has_down = z > 0

    def at(sp, tp):
        return {"device_id": (sp, tp), "device_id_type": MESH}

    barrier = pltpu.get_barrier_semaphore()
    ups, downs, side = (z + 1) * 2 + x, (z - 1) * 2 + x, z * 2 + 1 - x

    def greet(sp, tp):
        pl.semaphore_signal(barrier, inc=1, **at(sp, tp))

    pl.when(has_next)(lambda: greet(s + 1, t))
    pl.when(has_prev)(lambda: greet(s - 1, t))
    pl.when(has_up)(lambda: greet(ups, t))
    pl.when(has_down)(lambda: greet(downs, t))
    greet(side, t)
    for step in range(1, n_tp):
        greet(s, lax.rem(t + step, n_tp))

    loads = [
        pltpu.make_async_copy(source, target, load_sem.at[index])
        for index, (source, target) in enumerate(
            [
                (k_h.at[pl.ds(p * piece, piece)], col.at[z, 0, pl.ds(p * piece, piece)])
                for p in range(PIECES)
            ]
            + [
                (v_h.at[pl.ds(p * piece, piece)], col.at[z, 1, pl.ds(p * piece, piece)])
                for p in range(PIECES)
            ]
            + [
                (q_h, q),
                (mix_h, mix),
                (inp_h, inp),
                (gate_h, gate),
                (taps_h, taps),
                (gain_h, gain),
                (wc_h, wc),
                (wh_h, wh.at[pl.ds(a * wh_h.shape[0], wh_h.shape[0])]),
            ]
        )
    ]
    for load in loads:
        load.start()
    own_kv, (ld_q, ld_mix, ld_inp, ld_gate, ld_taps, ld_gain, ld_wc, ld_wh) = (
        loads[: 2 * PIECES],
        loads[2 * PIECES :],
    )

    pl.semaphore_wait(
        barrier,
        n_tp
        + has_next.astype(jnp.int32)
        + has_prev.astype(jnp.int32)
        + has_up.astype(jnp.int32)
        + has_down.astype(jnp.int32),
    )

    def part(blocks, level, p):
        return blocks.at[level, :, pl.ds(p * piece, piece), :]

    def up_copy(level, p):
        return pltpu.make_async_remote_copy(
            part(col, level, p), part(col, level, p), up_ss.at[level, p], col_rs.at[level, p], **at(ups, t)
        )

    def x_copy(level, p):
        return pltpu.make_async_remote_copy(
            part(col, level, p), part(cross, level, p), x_ss.at[level, p], cross_rs.at[level, p], **at(side, t)
        )

    def halo_copy(source, slot):
        return pltpu.make_async_remote_copy(
            source.at[pl.ds(rows - 16, 16)], halo.at[slot], halo_ss.at[slot], halo_rs.at[slot], **at(s + 1, t)
        )

    def forward(level, p, across=True):
        pl.when(has_up)(lambda: up_copy(level, p).start())
        if across is True:
            x_copy(level, p).start()
        else:
            pl.when(across)(lambda: x_copy(level, p).start())

    for p in range(PIECES):
        own_kv[p].wait()
        own_kv[PIECES + p].wait()
        forward(z, p, x == 0)

    ld_mix.wait()
    ld_inp.wait()

    @pl.when(has_next)
    def _():
        halo_copy(mix, 0).start()
        halo_copy(inp, 1).start()

    depth = wh_h.shape[0]
    late = LATE_TILES * COL_TILE
    early = width - late

    def w_copy(step):
        other = lax.rem(a + step, outer)
        mine = pl.ds(a * depth, depth)
        return pltpu.make_async_remote_copy(
            wh.at[mine, pl.ds(0, early)], wh.at[mine, pl.ds(0, early)], w_ss.at[step - 1], w_rs.at[step - 1], **at(s, other * 2 + b)
        )

    ld_wh.wait()
    for step in range(1, outer):
        w_copy(step).start()

    ld_q.wait()
    scale = HEAD_QK ** (-0.5)
    q[...] = (q[...].astype(F32) * scale).astype(BF16)

    def scores_of(block, m):
        lanes = slice(m * HEAD_QK, (m + 1) * HEAD_QK)
        return lax.dot_general(
            q[:, lanes], block[0, :, lanes], (((1,), (1,)), ((), ())), preferred_element_type=F32
        )

    ones = jnp.ones((rows, depth), BF16)

    def attend(block, first):
        tops, scored = [], []
        for m in range(2):
            scores = scores_of(block, m)
            if first:
                ahead = lax.broadcasted_iota(jnp.int32, scores.shape, 0)
                keys = lax.broadcasted_iota(jnp.int32, scores.shape, 1)
                scores = jnp.where(keys <= ahead, scores, -jnp.inf)
            top = jnp.max(scores, axis=1, keepdims=True)
            scored.append(scores)
            tops.append(top)
        for m in range(2):
            top = jnp.broadcast_to(tops[m], (rows, depth))
            if not first:
                before = peak[m]
                top = jnp.maximum(before, top)
                shrink = jnp.exp(before - top)
            wide = jnp.concatenate([top] * (rows // depth), axis=1) if rows > depth else top
            weights = jnp.exp(scored[m] - wide).astype(BF16)
            total = jnp.dot(weights, ones, preferred_element_type=F32)
            numer = jnp.dot(weights, block[1], preferred_element_type=F32)
            if not first:
                total = total + denom[m] * shrink
                numer = numer + acc[m] * shrink
            peak[m] = top
            denom[m] = total
            acc[m] = numer

    def attend_two(left, right):
        scored = [[scores_of(block, m) for block in (left, right)] for m in range(2)]
        tops = [
            jnp.max(jnp.maximum(scored[m][0], scored[m][1]), axis=1, keepdims=True) for m in range(2)
        ]
        for m in range(2):
            before = peak[m]
            top = jnp.maximum(before, jnp.broadcast_to(tops[m], (rows, depth)))
            shrink = jnp.exp(before - top)
            wide = jnp.concatenate([top] * (rows // depth), axis=1) if rows > depth else top
            total = denom[m] * shrink
            numer = acc[m] * shrink
            for scores, block in zip(scored[m], (left, right)):
                weights = jnp.exp(scores - wide).astype(BF16)
                total = total + jnp.dot(weights, ones, preferred_element_type=F32)
                numer = numer + jnp.dot(weights, block[1], preferred_element_type=F32)
            peak[m] = top
            denom[m] = total
            acc[m] = numer

    attend(col.at[z], True)

    ld_gate.wait()
    ld_taps.wait()
    ld_gain.wait()

    def gated(u, v):
        return (u.astype(F32) * v.astype(F32)).astype(BF16).astype(F32)

    ext[pl.ds(8, rows), :] = gated(mix[...], inp[...])

    @pl.when(has_prev)
    def _():
        halo_copy(mix, 0).wait_recv()
        halo_copy(inp, 1).wait_recv()
        ext[pl.ds(0, 8), :] = gated(halo[0], halo[1])[8:16]

    @pl.when(jnp.logical_not(has_prev))
    def _():
        ext[pl.ds(0, 8), :] = jnp.zeros((8, ext.shape[1]), F32)

    taps_v = taps[...].astype(F32)
    conv[...] = (
        gate[...].astype(F32)
        * (
            taps_v[0:1] * ext[pl.ds(6, rows), :]
            + taps_v[1:2] * ext[pl.ds(7, rows), :]
            + taps_v[2:3] * ext[pl.ds(8, rows), :]
        )
    ).astype(BF16)

    ld_wc.wait()
    partner = a * 2 + 1 - b

    def rows_of(oa, ob):
        return pl.ds(pl.multiple_of((oa * 2 + ob) * chunk, chunk), chunk)

    tiles = [slice(c, c + COL_TILE) for c in range(0, width, COL_TILE)]
    early_tiles, late_tiles = tiles[:-LATE_TILES], tiles[-LATE_TILES:]

    def cx_copy(step):
        return pltpu.make_async_remote_copy(
            cxs.at[step - 1], cxr.at[step - 1], cx_ss.at[step - 1], cx_rs.at[step - 1], **at(s, partner)
        )

    def cy_copy(step):
        other = lax.rem(a + step, outer)
        return pltpu.make_async_remote_copy(
            cys.at[step - 1], cyr.at[step - 1], cy_ss.at[step - 1], cy_rs.at[step - 1], **at(s, other * 2 + b)
        )

    for step in range(1, outer):
        other = lax.rem(a + step, outer)
        for tile in early_tiles:
            cxs[step - 1, :, tile] = jnp.dot(
                conv[rows_of(other, 1 - b), :], wc[:, tile], preferred_element_type=F32
            ).astype(BF16)
        cx_copy(step).start()

    def send_conv():
        for step in range(1, outer):
            other = lax.rem(a + step, outer)
            cx_copy(step).wait_recv()
            for tile in early_tiles:
                cys[step - 1, :, tile] = (
                    jnp.dot(conv[rows_of(other, b), :], wc[:, tile], preferred_element_type=F32)
                    + cxr[step - 1, :, tile].astype(F32)
                ).astype(BF16)
            cy_copy(step).start()

    pl.when(z == 0)(send_conv)

    def take_cross(level):
        for p in range(PIECES):
            x_copy(level, p).wait_recv()
        attend(cross.at[level], False)

    def advance(k, carry):
        level = z - k
        for p in range(PIECES):
            up_copy(level, p).wait_recv()
            forward(level, p)
        pl.when(k == 1)(send_conv)

        @pl.when(jnp.logical_or(k > 1, x == 1))
        def _():
            for p in range(PIECES):
                x_copy(level + 1, p).wait_recv()
            attend_two(cross.at[level + 1], col.at[level])

        pl.when(jnp.logical_and(k == 1, x == 0))(lambda: attend(col.at[level], False))
        return carry

    lax.fori_loop(1, z + 1, advance, 0)
    pl.when(jnp.logical_or(z > 0, x == 1))(lambda: take_cross(0))

    def merge(oa):
        chosen = pl.ds(pl.multiple_of(oa * 2 * chunk, 2 * chunk), 2 * chunk)
        merged = acc[0, chosen, :] / denom[0, chosen, :] - lam_ref[0] * (
            acc[1, chosen, :] / denom[1, chosen, :]
        )
        norm = lax.rsqrt(jnp.mean(merged * merged, axis=1, keepdims=True) + 1e-06)
        head[chosen, :] = (merged * norm * gain[...] * 0.8).astype(BF16)

    def ha_copy(step):
        other = lax.rem(a + step, outer)
        lanes = pl.ds(pl.multiple_of(a * depth, depth), depth)
        return pltpu.make_async_remote_copy(
            head.at[pl.ds(pl.multiple_of(other * 2 * chunk, 2 * chunk), 2 * chunk)],
            hact.at[:, lanes],
            ha_ss.at[step - 1],
            ha_rs.at[step - 1],
            **at(s, other * 2 + b),
        )

    for step in range(1, outer):
        merge(lax.rem(a + step, outer))
        ha_copy(step).start()
    merge(a)
    hact[:, pl.ds(pl.multiple_of(a * depth, depth), depth)] = head[
        pl.ds(pl.multiple_of(a * 2 * chunk, 2 * chunk), 2 * chunk), :
    ]
    held = pl.ds(pl.multiple_of(a * depth, depth), depth)

    def py_copy(step, ob):
        other = lax.rem(a + step, outer)
        return pltpu.make_async_remote_copy(
            pys.at[step - 1, ob],
            pyr.at[step - 1, b],
            py_ss.at[step - 1, ob],
            py_rs.at[step - 1, b],
            **at(s, other * 2 + ob),
        )

    def py_arrival(step, ob):
        return pltpu.make_async_remote_copy(
            pys.at[step - 1, ob],
            pyr.at[step - 1, ob],
            py_ss.at[step - 1, ob],
            py_rs.at[step - 1, ob],
            **at(s, lax.rem(a + step, outer) * 2 + ob),
        )

    def local(chosen, tile):
        return jnp.dot(conv[chosen, :], wc[:, tile], preferred_element_type=F32) + jnp.dot(
            head[chosen, :], wh[held, tile], preferred_element_type=F32
        )

    for step in range(1, outer):
        other = lax.rem(a + step, outer)
        for ob in range(2):
            for index, tile in enumerate(late_tiles):
                pys[step - 1, ob, :, index * COL_TILE : (index + 1) * COL_TILE] = local(
                    rows_of(other, ob), tile
                ).astype(BF16)
            py_copy(step, ob).start()
    for step in range(1, outer):
        w_copy(step).wait_recv()
    for step in range(1, outer):
        ha_copy(step).wait_recv()

    def fx_copy(index):
        lanes = tiles[index]
        return pltpu.make_async_remote_copy(
            fxs.at[:, lanes], fxr.at[:, lanes], fx_ss.at[index], fx_rs.at[index], **at(s, partner)
        )

    def contribution(ob, tile):
        mine = pl.ds(pl.multiple_of(ob * chunk, chunk), chunk)
        return jnp.dot(conv[rows_of(a, ob), :], wc[:, tile], preferred_element_type=F32) + jnp.dot(
            hact[mine, :], wh[:, tile], preferred_element_type=F32
        )

    def owed(ob, index):
        tile = tiles[index]
        return local(rows_of(a, ob), tile) if tile in late_tiles else contribution(ob, tile)

    order = list(range(len(early_tiles), len(tiles))) + list(range(len(early_tiles)))
    for index in order:
        fxs[:, tiles[index]] = owed(1 - b, index).astype(BF16)
        fx_copy(index).start()
    for step in range(1, outer):
        cy_copy(step).wait_recv()
    for index in order:
        tile = tiles[index]
        total = owed(b, index)
        if tile in early_tiles:
            for step in range(1, outer):
                total = total + cyr[step - 1, :, tile].astype(F32)
        own[:, tile] = total
    for step in range(1, outer):
        for ob in range(2):
            py_arrival(step, ob).wait_recv()
    for index in order:
        tile = tiles[index]
        total = own[:, tile]
        if tile in late_tiles:
            at_late = (index - len(early_tiles)) * COL_TILE
            for step in range(1, outer):
                for ob in range(2):
                    total = total + pyr[step - 1, ob, :, at_late : at_late + COL_TILE].astype(F32)
        fx_copy(index).wait_recv()
        out_ref[:, tile] = (total + fxr[:, tile].astype(F32)).astype(out_ref.dtype)

    def drain(level, carry):
        for p in range(PIECES):
            pl.when(has_up)(lambda: up_copy(level, p).wait_send())
            pl.when(jnp.logical_or(level < z, x == 0))(lambda: x_copy(level, p).wait_send())
        return carry

    lax.fori_loop(0, z + 1, drain, 0)

    @pl.when(has_next)
    def _():
        halo_copy(mix, 0).wait_send()
        halo_copy(inp, 1).wait_send()

    for step in range(1, outer):
        w_copy(step).wait_send()
        cx_copy(step).wait_send()
        cy_copy(step).wait_send()
        ha_copy(step).wait_send()
        for ob in range(2):
            py_copy(step, ob).wait_send()
    for index in range(len(tiles)):
        fx_copy(index).wait_send()


def shards(n_sp, n_tp, *args):
    gate, mix, inp, taps, q, k, v, lam, gain, wc, wh = args
    rows, lanes = q.shape
    depth, width = wh.shape
    levels, outer = n_sp // 2, n_tp // 2
    chunk = rows // n_tp
    tiles = width // COL_TILE
    late = LATE_TILES * COL_TILE
    dma = pltpu.SemaphoreType.DMA
    hbm = pl.BlockSpec(memory_space=pltpu.HBM)
    scratch = [
        pltpu.VMEM(gate.shape, BF16),
        pltpu.VMEM(mix.shape, BF16),
        pltpu.VMEM(inp.shape, BF16),
        pltpu.VMEM(taps.shape, BF16),
        pltpu.VMEM((1, gain.shape[0]), F32),
        pltpu.VMEM(q.shape, BF16),
        pltpu.VMEM((levels, 2, rows, lanes), BF16),
        pltpu.VMEM((levels, 2, rows, lanes), BF16),
        pltpu.VMEM((2, 16, mix.shape[1]), BF16),
        pltpu.VMEM((rows + 8, mix.shape[1]), F32),
        pltpu.VMEM(gate.shape, BF16),
        pltpu.VMEM(wc.shape, BF16),
        pltpu.VMEM((outer * depth, width), BF16),
        pltpu.VMEM((outer - 1, chunk, width - late), BF16),
        pltpu.VMEM((outer - 1, chunk, width - late), BF16),
        pltpu.VMEM((outer - 1, chunk, width - late), BF16),
        pltpu.VMEM((outer - 1, chunk, width - late), BF16),
        pltpu.VMEM((chunk, width), F32),
        pltpu.VMEM((chunk, width), BF16),
        pltpu.VMEM((chunk, width), BF16),
        pltpu.VMEM((rows, depth), BF16),
        pltpu.VMEM((2 * chunk, outer * depth), BF16),
        pltpu.VMEM((outer - 1, 2, chunk, late), BF16),
        pltpu.VMEM((outer - 1, 2, chunk, late), BF16),
        pltpu.VMEM((2, rows, depth), F32),
        pltpu.VMEM((2, rows, depth), F32),
        pltpu.VMEM((2, rows, depth), F32),
        dma((2 * PIECES + 8,)),
        dma((2,)),
        dma((2,)),
        dma((levels, PIECES)),
        dma((levels, PIECES)),
        dma((levels, PIECES)),
        dma((levels, PIECES)),
    ] + [dma((outer - 1,))] * 8 + [dma((tiles,))] * 2 + [dma((outer - 1, 2))] * 2
    return pl.pallas_call(
        functools.partial(kernel, n_sp, n_tp),
        out_shape=pltpu.VMEM((chunk, width), BF16),
        in_specs=[hbm] * 7 + [pl.BlockSpec(memory_space=pltpu.SMEM)] + [hbm] * 3,
        out_specs=pl.BlockSpec(memory_space=pltpu.VMEM),
        scratch_shapes=scratch,
        compiler_params=pltpu.CompilerParams(
            collective_id=0, has_side_effects=True, vmem_limit_bytes=66000000
        ),
    )(gate, mix, inp, taps, q, k, v, lam, gain.reshape(1, -1), wc, wh)


def solution(mesh):
    placed = (
        P("sp", "tp"),
        P("sp", "tp"),
        P("sp", "tp"),
        P(None, "tp"),
        P("sp", "tp"),
        P("sp", "tp"),
        P("sp", "tp"),
        P("tp"),
        P(),
        P("tp", None),
        P("tp", None),
    )
    return jax.shard_map(
        functools.partial(shards, mesh.shape["sp"], mesh.shape["tp"]),
        mesh=mesh,
        in_specs=placed,
        out_specs=P(("sp", "tp"), None),
        check_vma=False,
    )
```

```python
import functools

import jax
import jax.numpy as jnp
from jax import lax
from jax.experimental import pallas as pl
from jax.experimental.pallas import tpu as pltpu
from jax.sharding import PartitionSpec as P

HEAD_QK = 64
PIECES = 4
GROUPS = 4
UPWARD = (3,)
DOWNWARD = (0, 1)
COL_TILE = 512
MESH = pl.DeviceIdType.MESH
F32 = jnp.float32
BF16 = jnp.bfloat16


def kernel(
    n_sp,
    n_tp,
    gate_h,
    mix_h,
    inp_h,
    taps_h,
    q_h,
    k_h,
    v_h,
    lam_ref,
    gain_h,
    wc_h,
    wh_h,
    out_ref,
    gate,
    mix,
    inp,
    taps,
    gain,
    q,
    col,
    cross,
    halo,
    ext,
    conv,
    wc,
    wh,
    cys,
    cyr,
    own,
    head,
    heads,
    peak,
    acc,
    load_sem,
    halo_ss,
    halo_rs,
    up_ss,
    col_rs,
    x_ss,
    cross_rs,
    mate_ss,
    mate_rs,
    cy_ss,
    cy_rs,
    ha_ss,
    ha_rs,
    wy_ss,
    wy_rs,
    wz_ss,
    wz_rs,
    wf_ss,
    wf_rs,
):
    s = lax.axis_index("sp")
    t = lax.axis_index("tp")
    levels, outer = n_sp // 2, n_tp // 2
    z, x = s // 2, s % 2
    a, b = t // 2, t % 2
    mate = a * 2 + 1 - b
    rows, depth = q.shape
    width = out_ref.shape[1]
    chunk = rows // n_tp
    piece = rows // PIECES
    share = depth // GROUPS
    has_next = s < n_sp - 1
    has_prev = s > 0
    has_up = z < levels - 1
    has_down = z > 0
    paired = levels % 2 == 0
    odd = z % 2 == 1
    upward, downward = (UPWARD, DOWNWARD) if paired else ((), ())
    rest = tuple(g for g in range(GROUPS) if g not in upward + downward)
    even_groups, odd_groups = upward + rest, downward + rest

    def at(sp, tp):
        return {"device_id": (sp, tp), "device_id_type": MESH}

    barrier = pltpu.get_barrier_semaphore()
    ups, downs, side = (z + 1) * 2 + x, (z - 1) * 2 + x, z * 2 + 1 - x

    def greet(sp, tp):
        pl.semaphore_signal(barrier, inc=1, **at(sp, tp))

    pl.when(has_next)(lambda: greet(s + 1, t))
    pl.when(has_prev)(lambda: greet(s - 1, t))
    pl.when(has_up)(lambda: greet(ups, t))
    pl.when(has_down)(lambda: greet(downs, t))
    greet(side, t)
    for step in range(1, n_tp):
        greet(s, lax.rem(t + step, n_tp))

    def held(index, size=depth):
        return pl.ds(pl.multiple_of(index * size, size), size)

    kv = [(h.at[pl.ds(p * piece, piece)], col.at[z, i, pl.ds(p * piece, piece)]) for p in range(PIECES) for i, h in enumerate((k_h, v_h))]
    loads = [
        pltpu.make_async_copy(source, target, load_sem.at[index])
        for index, (source, target) in enumerate(
            [(mix_h, mix), (inp_h, inp)]
            + kv
            + [
                (q_h, q),
                (wh_h, wh.at[held(t)]),
                (wc_h, wc.at[held(b)]),
                (gate_h, gate),
                (taps_h, taps),
                (gain_h, gain),
            ]
        )
    ]
    for load in loads:
        load.start()
    ld_mix, ld_inp = loads[:2]
    own_kv = loads[2 : 2 + 2 * PIECES]
    ld_q, ld_wh, ld_wc, ld_gate, ld_taps, ld_gain = loads[2 + 2 * PIECES :]

    pl.semaphore_wait(
        barrier,
        n_tp
        + has_next.astype(jnp.int32)
        + has_prev.astype(jnp.int32)
        + has_up.astype(jnp.int32)
        + has_down.astype(jnp.int32),
    )

    def part(blocks, level, p):
        return blocks.at[level, :, pl.ds(p * piece, piece), :]

    def up_copy(level, p):
        return pltpu.make_async_remote_copy(
            part(col, level, p), part(col, level, p), up_ss.at[level, p], col_rs.at[level, p], **at(ups, t)
        )

    def x_copy(level, p):
        return pltpu.make_async_remote_copy(
            part(col, level, p), part(cross, level, p), x_ss.at[level, p], cross_rs.at[level, p], **at(side, t)
        )

    def halo_copy(source, slot):
        return pltpu.make_async_remote_copy(
            source.at[pl.ds(rows - 16, 16)], halo.at[slot], halo_ss.at[slot], halo_rs.at[slot], **at(s + 1, t)
        )

    def mate_copy(source, target, slot):
        return pltpu.make_async_remote_copy(source, target, mate_ss.at[slot], mate_rs.at[slot], **at(s, mate))

    def forward(level, p, across=True):
        pl.when(has_up)(lambda: up_copy(level, p).start())
        if across is True:
            x_copy(level, p).start()
        else:
            pl.when(across)(lambda: x_copy(level, p).start())

    ld_mix.wait()
    ld_inp.wait()

    @pl.when(has_next)
    def _():
        halo_copy(mix, 0).start()
        halo_copy(inp, 1).start()

    for p in range(PIECES):
        own_kv[2 * p].wait()
        own_kv[2 * p + 1].wait()
        forward(z, p, x == 0)

    steps = range(1, outer)

    def sent(g):
        return wh.at[held(t * GROUPS + g, share)]

    def theirs(step, g):
        source = lax.rem(a - step + outer, outer) * 2 + b
        return wh.at[held(source * GROUPS + g, share)]

    def wy_copy(step, g):
        other = lax.rem(a + step, outer)
        return pltpu.make_async_remote_copy(
            sent(g), sent(g), wy_ss.at[step - 1, g], wy_rs.at[step - 1, g], **at(s, other * 2 + b)
        )

    def wz_copy(step, g, target):
        ref = theirs(step, g)
        return pltpu.make_async_remote_copy(
            ref, ref, wz_ss.at[step - 1, g], wz_rs.at[step - 1, g], **at(target, t)
        )

    def wf_copy(step, g):
        ref = theirs(step, g)
        return pltpu.make_async_remote_copy(
            ref, ref, wf_ss.at[step - 1, g], wf_rs.at[step - 1, g], **at(s, mate)
        )

    def by_parity(on_odd, on_even):
        pl.when(odd)(on_odd)
        pl.when(jnp.logical_not(odd))(on_even)

    def send_groups(groups):
        def send():
            for g in groups:
                for step in steps:
                    wy_copy(step, g).start()

        return send

    wh_copy = mate_copy(wh.at[held(t)], wh.at[held(t)], 0)
    wc_copy = mate_copy(wc.at[held(b)], wc.at[held(b)], 1)
    lanes = pl.ds(pl.multiple_of(b * depth, depth), depth)
    conv_copy = mate_copy(conv.at[:, lanes], conv.at[:, lanes], 2)

    ld_wh.wait()
    by_parity(send_groups(odd_groups), send_groups(even_groups))
    ld_wc.wait()
    wc_copy.start()
    wh_copy.start()

    ld_q.wait()
    scale = HEAD_QK ** (-0.5)
    q[...] = (q[...].astype(F32) * scale).astype(BF16)

    def scores_of(block, m):
        pair = slice(m * HEAD_QK, (m + 1) * HEAD_QK)
        return lax.dot_general(
            q[:, pair], block[0, :, pair], (((1,), (1,)), ((), ())), preferred_element_type=F32
        )

    ones = jnp.ones((rows, depth), BF16)

    def spread(top, lanes_of):
        return jnp.concatenate([top] * (lanes_of // depth), axis=1) if lanes_of > depth else top

    def attend(blocks, first=False):
        scored = [[scores_of(block, m) for block in blocks] for m in range(2)]
        if first:
            ahead = lax.broadcasted_iota(jnp.int32, (rows, rows), 0)
            keys = lax.broadcasted_iota(jnp.int32, (rows, rows), 1)
            scored = [[jnp.where(keys <= ahead, scores, -jnp.inf) for scores in of] for of in scored]
        tops = [jnp.max(functools.reduce(jnp.maximum, of), axis=1, keepdims=True) for of in scored]
        for m in range(2):
            top = jnp.broadcast_to(tops[m], (rows, depth))
            if not first:
                before = peak[m]
                top = jnp.maximum(before, top)
                total = acc[m] * spread(jnp.exp(before - top), 2 * depth)
            wide = spread(top, rows)
            for index, (scores, block) in enumerate(zip(scored[m], blocks)):
                weights = jnp.exp(scores - wide).astype(BF16)
                add = jnp.dot(weights, jnp.concatenate([block[1], ones], axis=1), preferred_element_type=F32)
                total = add if first and index == 0 else total + add
            peak[m] = top
            acc[m] = total

    attend([col.at[z]], True)

    def gated(u, v):
        return (u.astype(F32) * v.astype(F32)).astype(BF16).astype(F32)

    def rows_of(oa, ob):
        return pl.ds(pl.multiple_of((oa * 2 + ob) * chunk, chunk), chunk)

    tiles = [slice(c, c + COL_TILE) for c in range(0, width, COL_TILE)]

    def cy_copy(step):
        other = lax.rem(a + step, outer)
        return pltpu.make_async_remote_copy(
            cys.at[step - 1], cyr.at[step - 1], cy_ss.at[step - 1], cy_rs.at[step - 1], **at(s, other * 2 + b)
        )

    def convolve():
        ext[pl.ds(8, rows), :] = gated(mix[...], inp[...])

        @pl.when(has_prev)
        def _():
            halo_copy(mix, 0).wait_recv()
            halo_copy(inp, 1).wait_recv()
            ext[pl.ds(0, 8), :] = gated(halo[0], halo[1])[8:16]

        @pl.when(jnp.logical_not(has_prev))
        def _():
            ext[pl.ds(0, 8), :] = jnp.zeros((8, ext.shape[1]), F32)

        ld_gate.wait()
        ld_taps.wait()
        taps_v = taps[...].astype(F32)
        conv[:, lanes] = (
            gate[...].astype(F32)
            * (
                taps_v[0:1] * ext[pl.ds(6, rows), :]
                + taps_v[1:2] * ext[pl.ds(7, rows), :]
                + taps_v[2:3] * ext[pl.ds(8, rows), :]
            )
        ).astype(BF16)
        conv_copy.start()

    def project_conv():
        wc_copy.wait_recv()
        conv_copy.wait_recv()
        for step in steps:
            other = lax.rem(a + step, outer)
            for tile in tiles:
                cys[step - 1, :, tile] = jnp.dot(
                    conv[rows_of(other, b), :], wc[:, tile], preferred_element_type=F32
                ).astype(BF16)
            cy_copy(step).start()
        for tile in tiles:
            own[:, tile] = jnp.dot(conv[rows_of(a, b), :], wc[:, tile], preferred_element_type=F32)

    def take(groups, target=None):
        for g in groups:
            for step in steps:
                wy_copy(step, g).wait_recv()
                if target is not None:
                    wz_copy(step, g, target).start()
                wf_copy(step, g).start()

    def take_from(groups, target):
        for g in groups:
            for step in steps:
                wz_copy(step, g, target).wait_recv()
                wf_copy(step, g).start()

    def stage_a():
        by_parity(lambda: take(downward[:1], downs), lambda: take(upward, ups))

    def stage_b():
        by_parity(lambda: take(downward[1:], downs), lambda: take(rest))

    def stage_c():
        by_parity(lambda: take(rest), lambda: take_from(downward, ups))

    def stage_d():
        pl.when(odd)(lambda: take_from(upward, downs))

    def convolve_s():
        convolve()

    def project_s():
        project_conv()

    @pl.when(z == 0)
    def _():
        convolve_s()
        project_s()

    def pieces(level, low, high):
        for p in range(low, high):
            up_copy(level, p).wait_recv()
            forward(level, p)

    def await_cross(level):
        for p in range(PIECES):
            x_copy(level, p).wait_recv()

    def attend_pair(level, crossed, both):
        @pl.when(both)
        def _():
            await_cross(crossed)
            attend([cross.at[crossed], col.at[level]])

        @pl.when(jnp.logical_not(both))
        def _():
            attend([col.at[level]])

    def advance(k, carry):
        level = z - k
        pieces(level, 0, PIECES // 2)
        pl.when(k > 1)(lambda: attend_pair(level + 1, jnp.minimum(level + 2, z), jnp.logical_or(k > 2, x == 1)))
        pl.when(k == 3)(stage_b)
        pieces(level, PIECES // 2, PIECES)
        pl.when(k == 1)(convolve_s)

        @pl.when(k == 2)
        def _():
            project_s()
            stage_a()

        return carry

    lax.fori_loop(1, z + 1, advance, 0)
    pl.when(z > 0)(lambda: attend_pair(0, jnp.minimum(1, z), jnp.logical_or(z > 1, x == 1)))

    @pl.when(z == 1)
    def _():
        project_s()
        stage_a()

    pl.when(jnp.logical_and(z > 0, z < 3))(stage_b)
    soon = jnp.logical_and(z > 2, odd)
    pl.when(soon)(stage_c)

    @pl.when(jnp.logical_or(z > 0, x == 1))
    def _():
        await_cross(0)
        attend([cross.at[0]])

    ld_gain.wait()

    def merge(oa):
        chosen = pl.ds(pl.multiple_of(oa * 2 * chunk, 2 * chunk), 2 * chunk)
        merged = acc[0, chosen, :depth] / acc[0, chosen, depth:] - lam_ref[0] * (
            acc[1, chosen, :depth] / acc[1, chosen, depth:]
        )
        norm = lax.rsqrt(jnp.mean(merged * merged, axis=1, keepdims=True) + 1e-06)
        head[chosen, :] = (merged * norm * gain[...] * 0.8).astype(BF16)

    mine = pl.ds(pl.multiple_of(t * depth, depth), depth)

    def ha_copy(step, ob):
        other = lax.rem(a + step, outer)
        return pltpu.make_async_remote_copy(
            head.at[rows_of(other, ob)],
            heads.at[:, mine],
            ha_ss.at[step - 1, ob],
            ha_rs.at[step - 1, b],
            **at(s, other * 2 + ob),
        )

    def ha_arrival(step, ob):
        return pltpu.make_async_remote_copy(
            head.at[rows_of(a, b)],
            heads.at[:, mine],
            ha_ss.at[step - 1, ob],
            ha_rs.at[step - 1, ob],
            **at(s, mate),
        )

    mate_head = mate_copy(head.at[rows_of(a, 1 - b)], heads.at[:, mine], 3)
    for step in steps:
        merge(lax.rem(a + step, outer))
        for ob in range(2):
            ha_copy(step, ob).start()
    merge(a)
    mate_head.start()
    heads[:, mine] = head[rows_of(a, b), :]

    @pl.when(z == 0)
    def _():
        stage_a()
        stage_b()

    pl.when(jnp.logical_not(soon))(stage_c)
    stage_d()

    def product(oa, tile):
        k = held(oa, 2 * depth)
        return jnp.dot(heads[:, k], wh[k, tile], preferred_element_type=F32)

    wh_copy.wait_recv()
    mate_head.wait_recv()
    for tile in tiles:
        own[:, tile] += product(a, tile)
    for step in steps:
        cy_copy(step).wait_recv()
    for step in steps:
        for g in range(GROUPS):
            wf_copy(step, g).wait_recv()
    for step in steps:
        for ob in range(2):
            ha_arrival(step, ob).wait_recv()
    for tile in tiles:
        total = own[:, tile]
        for step in steps:
            total = total + cyr[step - 1, :, tile].astype(F32) + product(lax.rem(a + step, outer), tile)
        out_ref[:, tile] = total.astype(out_ref.dtype)


    def drain(level, carry):
        for p in range(PIECES):
            pl.when(has_up)(lambda: up_copy(level, p).wait_send())
            pl.when(jnp.logical_or(level < z, x == 0))(lambda: x_copy(level, p).wait_send())
        return carry

    lax.fori_loop(0, z + 1, drain, 0)

    @pl.when(has_next)
    def _():
        halo_copy(mix, 0).wait_send()
        halo_copy(inp, 1).wait_send()

    def drain_groups(sent_groups, passed, target):
        def run():
            for step in steps:
                for g in sent_groups:
                    wy_copy(step, g).wait_send()
                for g in passed:
                    wz_copy(step, g, target).wait_send()

        return run

    by_parity(drain_groups(odd_groups, downward, downs), drain_groups(even_groups, upward, ups))
    for copy in (wh_copy, wc_copy, conv_copy, mate_head):
        copy.wait_send()
    for step in steps:
        for g in range(GROUPS):
            wf_copy(step, g).wait_send()
        cy_copy(step).wait_send()
        for ob in range(2):
            ha_copy(step, ob).wait_send()


def shards(n_sp, n_tp, *args):
    gate, mix, inp, taps, q, k, v, lam, gain, wc, wh = args
    rows, lanes = q.shape
    depth, width = wh.shape
    levels, outer = n_sp // 2, n_tp // 2
    chunk = rows // n_tp
    dma = pltpu.SemaphoreType.DMA
    hbm = pl.BlockSpec(memory_space=pltpu.HBM)
    scratch = [
        pltpu.VMEM(gate.shape, BF16),
        pltpu.VMEM(mix.shape, BF16),
        pltpu.VMEM(inp.shape, BF16),
        pltpu.VMEM(taps.shape, BF16),
        pltpu.VMEM((1, gain.shape[0]), F32),
        pltpu.VMEM(q.shape, BF16),
        pltpu.VMEM((levels, 2, rows, lanes), BF16),
        pltpu.VMEM((levels, 2, rows, lanes), BF16),
        pltpu.VMEM((2, 16, mix.shape[1]), BF16),
        pltpu.VMEM((rows + 8, mix.shape[1]), F32),
        pltpu.VMEM((rows, 2 * lanes), BF16),
        pltpu.VMEM((2 * depth, width), BF16),
        pltpu.VMEM((n_tp * depth, width), BF16),
        pltpu.VMEM((outer - 1, chunk, width), BF16),
        pltpu.VMEM((outer - 1, chunk, width), BF16),
        pltpu.VMEM((chunk, width), F32),
        pltpu.VMEM((rows, depth), BF16),
        pltpu.VMEM((chunk, n_tp * depth), BF16),
        pltpu.VMEM((2, rows, depth), F32),
        pltpu.VMEM((2, rows, 2 * depth), F32),
        dma((2 * PIECES + 8,)),
        dma((2,)),
        dma((2,)),
        dma((levels, PIECES)),
        dma((levels, PIECES)),
        dma((levels, PIECES)),
        dma((levels, PIECES)),
        dma((4,)),
        dma((4,)),
        dma((outer - 1,)),
        dma((outer - 1,)),
        dma((outer - 1, 2)),
        dma((outer - 1, 2)),
    ] + [dma((outer - 1, GROUPS))] * 6
    return pl.pallas_call(
        functools.partial(kernel, n_sp, n_tp),
        out_shape=pltpu.VMEM((chunk, width), BF16),
        in_specs=[hbm] * 7 + [pl.BlockSpec(memory_space=pltpu.SMEM)] + [hbm] * 3,
        out_specs=pl.BlockSpec(memory_space=pltpu.VMEM),
        scratch_shapes=scratch,
        compiler_params=pltpu.CompilerParams(
            collective_id=0, has_side_effects=True, vmem_limit_bytes=66000000
        ),
    )(gate, mix, inp, taps, q, k, v, lam, gain.reshape(1, -1), wc, wh)


def solution(mesh):
    placed = (
        P("sp", "tp"),
        P("sp", "tp"),
        P("sp", "tp"),
        P(None, "tp"),
        P("sp", "tp"),
        P("sp", "tp"),
        P("sp", "tp"),
        P("tp"),
        P(),
        P("tp", None),
        P("tp", None),
    )
    return jax.shard_map(
        functools.partial(shards, mesh.shape["sp"], mesh.shape["tp"]),
        mesh=mesh,
        in_specs=placed,
        out_specs=P(("sp", "tp"), None),
        check_vma=False,
    )
```

```python
import functools

import jax
import jax.numpy as jnp
from jax import lax
from jax.experimental import pallas as pl
from jax.experimental.pallas import tpu as pltpu
from jax.sharding import PartitionSpec as P

HEAD_QK = 64
PIECES = 4
GROUPS = 4
UPWARD = (3,)
DOWNWARD = (0, 1)
COL_TILE = 512
MESH = pl.DeviceIdType.MESH
F32 = jnp.float32
BF16 = jnp.bfloat16


def kernel(
    n_sp,
    n_tp,
    gate_h,
    mix_h,
    inp_h,
    taps_h,
    q_h,
    k_h,
    v_h,
    lam_ref,
    gain_h,
    wc_h,
    wh_h,
    out_ref,
    mi,
    qg,
    taps,
    gain,
    col,
    cross,
    halo,
    relay,
    ext,
    conv,
    wc,
    wh,
    cys,
    cyr,
    own,
    head,
    heads,
    peak,
    acc,
    load_sem,
    halo_ss,
    halo_rs,
    up_ss,
    col_rs,
    x_ss,
    cross_rs,
    ex_ss,
    eu_ss,
    e_rs,
    mate_ss,
    mate_rs,
    cy_ss,
    cy_rs,
    ha_ss,
    ha_rs,
    wy_ss,
    wy_rs,
    wz_ss,
    wz_rs,
    wf_ss,
    wf_rs,
):
    s = lax.axis_index("sp")
    t = lax.axis_index("tp")
    levels, outer = n_sp // 2, n_tp // 2
    z, x = s // 2, s % 2
    a, b = t // 2, t % 2
    mate = a * 2 + 1 - b
    _, rows, depth = qg.shape
    mix, inp, q, gate = mi.at[0], mi.at[1], qg.at[0], qg.at[1]
    half = rows // 2
    width = out_ref.shape[1]
    chunk = rows // n_tp
    piece = rows // PIECES
    share = depth // GROUPS
    has_prev = s > 0
    has_up = z < levels - 1
    has_down = z > 0
    paired = levels % 2 == 0
    odd = z % 2 == 1
    upward, downward = (UPWARD, DOWNWARD) if paired else ((), ())
    rest = tuple(g for g in range(GROUPS) if g not in upward + downward)
    even_groups, odd_groups = upward + rest, downward + rest

    def at(sp, tp):
        return {"device_id": (sp, tp), "device_id_type": MESH}

    barrier = pltpu.get_barrier_semaphore()
    ups, downs, side = (z + 1) * 2 + x, (z - 1) * 2 + x, z * 2 + 1 - x

    def greet(sp, tp):
        pl.semaphore_signal(barrier, inc=1, **at(sp, tp))

    pl.when(has_up)(lambda: greet(ups, t))
    pl.when(has_down)(lambda: greet(downs, t))
    greet(side, t)
    for step in range(1, n_tp):
        greet(s, lax.rem(t + step, n_tp))

    def held(index, size=depth):
        return pl.ds(pl.multiple_of(index * size, size), size)

    loads = [
        pltpu.make_async_copy(source, target, load_sem.at[index])
        for source, target, index in (
            (k_h, col.at[z, 0], 0),
            (v_h, col.at[z, 1], 0),
            (mix_h, mix, 1),
            (inp_h, inp, 1),
            (q_h, q, 2),
            (gate_h, gate, 2),
            (wh_h, wh.at[held(t)], 3),
            (wc_h, wc.at[held(b)], 4),
            (taps_h, taps, 5),
            (gain_h, gain, 6),
        )
    ]
    for load in loads:
        load.start()
    ld_wh, ld_wc, ld_taps, ld_gain = loads[6:]

    def loaded(both, index):
        return pltpu.make_async_copy(both, both, load_sem.at[index])

    pl.semaphore_wait(barrier, n_tp + has_up.astype(jnp.int32) + has_down.astype(jnp.int32))

    def part(blocks, level, p):
        return blocks.at[level, :, pl.ds(p * piece, piece), :]

    def up_copy(level, p):
        return pltpu.make_async_remote_copy(
            part(col, level, p), part(col, level, p), up_ss.at[level], col_rs.at[level, p], **at(ups, t)
        )

    def up_all(level):
        return pltpu.make_async_remote_copy(
            col.at[level], col.at[level], up_ss.at[level], col_rs.at[level, 0], **at(ups, t)
        )

    def x_copy(level, p):
        return pltpu.make_async_remote_copy(
            part(col, level, p), part(cross, level, p), x_ss.at[level], cross_rs.at[level], **at(side, t)
        )

    def x_all(level):
        return pltpu.make_async_remote_copy(
            col.at[level], cross.at[level], x_ss.at[level], cross_rs.at[level], **at(side, t)
        )

    first_half = pl.ds(0, half)

    def x_half(level):
        return pltpu.make_async_remote_copy(
            col.at[level, :, first_half, :], cross.at[level, :, first_half, :], x_ss.at[level], cross_rs.at[level], **at(side, t)
        )

    early, extra = range(PIECES // 2), range(PIECES // 2, PIECES)

    def ex_copy(p):
        return pltpu.make_async_remote_copy(
            part(col, 0, p), part(cross, 0, p), ex_ss.at[0], e_rs.at[p - PIECES // 2], **at(side, t)
        )

    def eu_copy(p):
        ref = part(cross, 0, p)
        return pltpu.make_async_remote_copy(ref, ref, eu_ss.at[0], e_rs.at[p - PIECES // 2], **at(ups, t))

    def half_sent(sem):
        ref = cross.at[0, :, first_half, :]
        return pltpu.make_async_remote_copy(ref, ref, sem.at[0], e_rs.at[0], **at(side, t))

    edge = mi.at[:, pl.ds(rows - 16, 16), :]

    def halo_copy(source, target, slot, to):
        return pltpu.make_async_remote_copy(source, target, halo_ss.at[slot], halo_rs.at[slot], **at(to, t))

    halo_side = halo_copy(edge, halo, 0, side)
    halo_up = halo_copy(edge, relay, 1, ups)
    halo_pass = halo_copy(relay, halo, 0, side)

    def mate_copy(source, target, slot):
        return pltpu.make_async_remote_copy(source, target, mate_ss.at[max(slot - 1, 0)], mate_rs.at[slot], **at(s, mate))

    def forward(level, p):
        pl.when(has_up)(lambda: up_copy(level, p).start())
        if p in early:
            x_copy(level, p).start()
        else:
            pl.when(level > 0)(lambda: x_copy(level, p).start())

    loaded(mi, 1).wait()
    pl.when(x == 0)(lambda: halo_side.start())
    pl.when(jnp.logical_and(x == 1, has_up))(lambda: halo_up.start())
    loaded(col.at[z], 0).wait()

    @pl.when(has_up)
    def _():
        for p in range(PIECES):
            up_copy(z, p).start()

    @pl.when(z == 0)
    def _():
        for p in extra:
            ex_copy(p).start()

    @pl.when(x == 0)
    def _():
        for p in early:
            x_copy(z, p).start()

        @pl.when(z > 0)
        def _():
            for p in extra:
                x_copy(z, p).start()

    steps = range(1, outer)

    def sent(g):
        return wh.at[held(t * GROUPS + g, share)]

    def wy_copy(step, g, place):
        other = lax.rem(a + step, outer)
        return pltpu.make_async_remote_copy(
            sent(g), sent(g), wy_ss.at[step - 1], wy_rs.at[step - 1, place], **at(s, other * 2 + b)
        )

    def region(index, groups):
        return wh.at[pl.ds(pl.multiple_of(index * depth + groups[0] * share, share), len(groups) * share)]

    def source_of(step):
        return lax.rem(a - step + outer, outer) * 2 + b

    def wy_sent(step, groups):
        ref = region(t, sorted(groups))
        return pltpu.make_async_remote_copy(ref, ref, wy_ss.at[step - 1], wy_rs.at[step - 1, 0], **at(s, mate))

    def wz_copy(step, groups, target):
        ref = region(source_of(step), groups)
        return pltpu.make_async_remote_copy(ref, ref, wz_ss.at[step - 1], wz_rs.at[step - 1], **at(target, t))

    def wf_copy(step, groups):
        ref = region(source_of(step), groups)
        return pltpu.make_async_remote_copy(ref, ref, wf_ss.at[step - 1], wf_rs.at[step - 1], **at(s, mate))

    def by_parity(on_odd, on_even):
        pl.when(odd)(on_odd)
        pl.when(jnp.logical_not(odd))(on_even)

    def send_groups(groups):
        def send():
            for place, g in enumerate(groups):
                for step in steps:
                    wy_copy(step, g, place).start()

        return send

    wh_copy = mate_copy(wh.at[held(t)], wh.at[held(t)], 0)
    wc_copy = mate_copy(wc.at[held(b)], wc.at[held(b)], 1)
    lanes = pl.ds(pl.multiple_of(b * depth, depth), depth)
    conv_copy = mate_copy(conv.at[:, lanes], conv.at[:, lanes], 2)

    ld_wh.wait()
    by_parity(send_groups(odd_groups), send_groups(even_groups))
    ld_wc.wait()
    wc_copy.start()
    wh_copy.start()

    @pl.when(jnp.logical_and(x == 1, z > 0))
    def _():
        halo_up.wait_recv()
        halo_pass.start()

    loaded(qg, 2).wait()
    scale = HEAD_QK ** (-0.5)
    q[...] = (q[...].astype(F32) * scale).astype(BF16)

    def scores_of(block, m):
        pair = slice(m * HEAD_QK, (m + 1) * HEAD_QK)
        return lax.dot_general(
            q[:, pair], block[0, :, pair], (((1,), (1,)), ((), ())), preferred_element_type=F32
        )

    ones = jnp.ones((rows, depth), BF16)

    def spread(top, lanes_of):
        return jnp.concatenate([top] * (lanes_of // depth), axis=1) if lanes_of > depth else top

    def attend(blocks, first=False):
        scored = [[scores_of(block, m) for block in blocks] for m in range(2)]
        if first:
            ahead = lax.broadcasted_iota(jnp.int32, (rows, rows), 0)
            keys = lax.broadcasted_iota(jnp.int32, (rows, rows), 1)
            scored = [[jnp.where(keys <= ahead, scores, -jnp.inf) for scores in of] for of in scored]
        tops = [jnp.max(functools.reduce(jnp.maximum, of), axis=1, keepdims=True) for of in scored]
        for m in range(2):
            top = jnp.broadcast_to(tops[m], (rows, depth))
            if not first:
                before = peak[m]
                top = jnp.maximum(before, top)
                total = acc[m] * spread(jnp.exp(before - top), 2 * depth)
            wide = spread(top, rows)
            for index, (scores, block) in enumerate(zip(scored[m], blocks)):
                weights = jnp.exp(scores - wide).astype(BF16)
                add = jnp.dot(weights, jnp.concatenate([block[1], ones], axis=1), preferred_element_type=F32)
                total = add if first and index == 0 else total + add
            peak[m] = top
            acc[m] = total

    attend([col.at[z]], True)

    def gated(u, v):
        return (u.astype(F32) * v.astype(F32)).astype(BF16).astype(F32)

    def rows_of(oa, ob):
        return pl.ds(pl.multiple_of((oa * 2 + ob) * chunk, chunk), chunk)

    tiles = [slice(c, c + COL_TILE) for c in range(0, width, COL_TILE)]

    def cy_copy(step):
        other = lax.rem(a + step, outer)
        return pltpu.make_async_remote_copy(
            cys.at[step - 1], cyr.at[step - 1], cy_ss.at[step - 1], cy_rs.at[step - 1], **at(s, other * 2 + b)
        )

    def convolve():
        ext[pl.ds(8, rows), :] = gated(mix[...], inp[...])

        @pl.when(has_prev)
        def _():
            halo_side.wait_recv()
            ext[pl.ds(0, 8), :] = gated(halo[0], halo[1])[8:16]

        @pl.when(jnp.logical_not(has_prev))
        def _():
            ext[pl.ds(0, 8), :] = jnp.zeros((8, ext.shape[1]), F32)

        ld_taps.wait()
        taps_v = taps[...].astype(F32)
        conv[:, lanes] = (
            gate[...].astype(F32)
            * (
                taps_v[0:1] * ext[pl.ds(6, rows), :]
                + taps_v[1:2] * ext[pl.ds(7, rows), :]
                + taps_v[2:3] * ext[pl.ds(8, rows), :]
            )
        ).astype(BF16)
        conv_copy.start()

    def project_conv():
        wc_copy.wait_recv()
        conv_copy.wait_recv()
        for step in steps:
            other = lax.rem(a + step, outer)
            for tile in tiles:
                cys[step - 1, :, tile] = jnp.dot(
                    conv[rows_of(other, b), :], wc[:, tile], preferred_element_type=F32
                ).astype(BF16)
            cy_copy(step).start()
        for tile in tiles:
            own[:, tile] = jnp.dot(conv[rows_of(a, b), :], wc[:, tile], preferred_element_type=F32)

    def take(groups, order, passed=None):
        for g in groups:
            for step in steps:
                wy_copy(step, g, order.index(g)).wait_recv()
                if passed is not None:
                    wz_copy(step, (g,), passed).start()
                wf_copy(step, (g,)).start()

    def take_from(groups, target):
        for step in steps if groups else ():
            wz_copy(step, groups, target).wait_recv()
            wf_copy(step, groups).start()

    def odd_a():
        take(downward[:1], odd_groups, downs)

    def odd_b():
        take(downward[1:], odd_groups, downs)

    def odd_c():
        take(rest, odd_groups)

    def odd_d():
        take_from(upward, downs)

    def even_a():
        take(upward, even_groups, ups)

    def even_b():
        take(rest, even_groups)

    def even_c():
        take_from(downward, ups)

    def extras():
        for p in extra:
            eu_copy(p).wait_recv()
            pl.when(has_up)(lambda: eu_copy(p).start())

    def convolve_s():
        convolve()

    def project_s():
        project_conv()

    @pl.when(z == 0)
    def _():
        extras()
        convolve_s()
        project_s()

    def pieces(level, low, high):
        for p in range(low, high):
            up_copy(level, p).wait_recv()
            forward(level, p)

    def await_cross(level):
        x_all(level).wait_recv()

    def attend_pair(level, crossed, both):
        @pl.when(both)
        def _():
            await_cross(crossed)
            attend([cross.at[crossed], col.at[level]])

        @pl.when(jnp.logical_not(both))
        def _():
            attend([col.at[level]])

    def advance(k, carry):
        level = z - k
        pieces(level, 0, PIECES // 2)
        pl.when(jnp.logical_and(k == 3, odd))(odd_b)
        pl.when(k > 1)(lambda: attend_pair(level + 1, jnp.minimum(level + 2, z), jnp.logical_or(k > 2, x == 1)))
        pl.when(jnp.logical_and(k == 2, odd))(odd_a)
        pieces(level, PIECES // 2, PIECES)
        pl.when(k == 1)(convolve_s)
        pl.when(k == 2)(project_s)

        return carry

    lax.fori_loop(1, z + 1, advance, 0)

    @pl.when(z > 0)
    def _():
        attend_pair(0, jnp.minimum(1, z), jnp.logical_or(z > 1, x == 1))
        pl.when(z == 1)(odd_a)
        extras()

    @pl.when(z == 1)
    def _():
        project_s()
        odd_b()

    @pl.when(jnp.logical_and(z > 1, jnp.logical_not(odd)))
    def _():
        even_a()
        even_b()

    soon = jnp.logical_and(z > 2, odd)
    pl.when(soon)(odd_c)

    @pl.when(jnp.logical_or(z > 0, x == 1))
    def _():
        x_half(0).wait_recv()
        attend([cross.at[0]])

    ld_gain.wait()

    def merge(oa):
        chosen = pl.ds(pl.multiple_of(oa * 2 * chunk, 2 * chunk), 2 * chunk)
        merged = acc[0, chosen, :depth] / acc[0, chosen, depth:] - lam_ref[0] * (
            acc[1, chosen, :depth] / acc[1, chosen, depth:]
        )
        norm = lax.rsqrt(jnp.mean(merged * merged, axis=1, keepdims=True) + 1e-06)
        head[chosen, :] = (merged * norm * gain[...] * 0.8).astype(BF16)

    mine = pl.ds(pl.multiple_of(t * depth, depth), depth)

    def ha_copy(step, ob):
        other = lax.rem(a + step, outer)
        return pltpu.make_async_remote_copy(
            head.at[rows_of(other, ob)],
            heads.at[:, mine],
            ha_ss.at[step - 1],
            ha_rs.at[step - 1],
            **at(s, other * 2 + ob),
        )

    def ha_sent(step):
        ref = head.at[pl.ds(pl.multiple_of(lax.rem(a + step, outer) * 2 * chunk, 2 * chunk), 2 * chunk)]
        return pltpu.make_async_remote_copy(ref, ref, ha_ss.at[step - 1], ha_rs.at[step - 1], **at(s, mate))

    def ha_arrival(step):
        ref = heads.at[:, held(lax.rem(a - step + outer, outer), 2 * depth)]
        return pltpu.make_async_remote_copy(ref, ref, ha_ss.at[step - 1], ha_rs.at[step - 1], **at(s, mate))

    mate_head = mate_copy(head.at[rows_of(a, 1 - b)], heads.at[:, mine], 3)
    for step in steps:
        merge(lax.rem(a + step, outer))
        for ob in range(2):
            ha_copy(step, ob).start()
    merge(a)
    mate_head.start()
    heads[:, mine] = head[rows_of(a, b), :]

    @pl.when(z == 0)
    def _():
        even_a()
        even_b()

    def odd_end():
        pl.when(z < 3)(odd_c)
        odd_d()

    by_parity(odd_end, even_c)

    def product(oa, tile):
        k = held(oa, 2 * depth)
        return jnp.dot(heads[:, k], wh[k, tile], preferred_element_type=F32)

    wh_copy.wait_recv()
    mate_head.wait_recv()
    for tile in tiles:
        own[:, tile] += product(a, tile)
    for step in steps:
        cy_copy(step).wait_recv()
    for step in steps:
        wf_copy(step, tuple(range(GROUPS))).wait_recv()
    for step in steps:
        ha_arrival(step).wait_recv()
    for tile in tiles:
        total = own[:, tile]
        for step in steps:
            total = total + cyr[step - 1, :, tile].astype(F32) + product(lax.rem(a + step, outer), tile)
        out_ref[:, tile] = total.astype(out_ref.dtype)


    def drain(level, carry):
        pl.when(has_up)(lambda: up_all(level).wait_send())
        pl.when(jnp.logical_and(level > 0, jnp.logical_or(level < z, x == 0)))(lambda: x_all(level).wait_send())
        return carry

    lax.fori_loop(0, z + 1, drain, 0)
    pl.when(jnp.logical_or(z > 0, x == 0))(lambda: x_half(0).wait_send())
    pl.when(z == 0)(lambda: half_sent(ex_ss).wait_send())
    pl.when(has_up)(lambda: half_sent(eu_ss).wait_send())
    pl.when(x == 0)(lambda: halo_side.wait_send())
    pl.when(jnp.logical_and(x == 1, has_up))(lambda: halo_up.wait_send())
    pl.when(jnp.logical_and(x == 1, z > 0))(lambda: halo_pass.wait_send())

    def drain_groups(sent_groups, passed, target):
        def run():
            for step in steps:
                wy_sent(step, sent_groups).wait_send()
                if passed:
                    wz_copy(step, passed, target).wait_send()

        return run

    by_parity(drain_groups(odd_groups, downward, downs), drain_groups(even_groups, upward, ups))
    mate_copy(wc, wc, 0).wait_send()
    conv_copy.wait_send()
    mate_head.wait_send()
    for step in steps:
        wf_copy(step, tuple(range(GROUPS))).wait_send()
        cy_copy(step).wait_send()
        ha_sent(step).wait_send()


def shards(n_sp, n_tp, *args):
    gate, mix, inp, taps, q, k, v, lam, gain, wc, wh = args
    rows, lanes = q.shape
    depth, width = wh.shape
    levels, outer = n_sp // 2, n_tp // 2
    chunk = rows // n_tp
    dma = pltpu.SemaphoreType.DMA
    hbm = pl.BlockSpec(memory_space=pltpu.HBM)
    scratch = [
        pltpu.VMEM((2, rows, lanes), BF16),
        pltpu.VMEM((2, rows, lanes), BF16),
        pltpu.VMEM(taps.shape, BF16),
        pltpu.VMEM((1, gain.shape[0]), F32),
        pltpu.VMEM((levels, 2, rows, lanes), BF16),
        pltpu.VMEM((levels, 2, rows, lanes), BF16),
        pltpu.VMEM((2, 16, lanes), BF16),
        pltpu.VMEM((2, 16, lanes), BF16),
        pltpu.VMEM((rows + 8, lanes), F32),
        pltpu.VMEM((rows, 2 * lanes), BF16),
        pltpu.VMEM((2 * depth, width), BF16),
        pltpu.VMEM((n_tp * depth, width), BF16),
        pltpu.VMEM((outer - 1, chunk, width), BF16),
        pltpu.VMEM((outer - 1, chunk, width), BF16),
        pltpu.VMEM((chunk, width), F32),
        pltpu.VMEM((rows, depth), BF16),
        pltpu.VMEM((chunk, n_tp * depth), BF16),
        pltpu.VMEM((2, rows, depth), F32),
        pltpu.VMEM((2, rows, 2 * depth), F32),
        dma((7,)),
        dma((2,)),
        dma((2,)),
        dma((max(levels - 1, 1),)),
        dma((max(levels - 1, 1), PIECES)),
        dma((levels,)),
        dma((levels,)),
        dma((1,)),
        dma((1,)),
        dma((PIECES // 2,)),
        dma((3,)),
        dma((4,)),
        dma((outer - 1,)),
        dma((outer - 1,)),
        dma((outer - 1,)),
        dma((outer - 1,)),
        dma((outer - 1,)),
        dma((outer - 1, GROUPS - min(len(UPWARD), len(DOWNWARD)) if levels % 2 == 0 else GROUPS)),
    ] + [dma((outer - 1,))] * 4
    return pl.pallas_call(
        functools.partial(kernel, n_sp, n_tp),
        out_shape=pltpu.VMEM((chunk, width), BF16),
        in_specs=[hbm] * 7 + [pl.BlockSpec(memory_space=pltpu.SMEM)] + [hbm] * 3,
        out_specs=pl.BlockSpec(memory_space=pltpu.VMEM),
        scratch_shapes=scratch,
        compiler_params=pltpu.CompilerParams(
            collective_id=0, has_side_effects=True, vmem_limit_bytes=66000000
        ),
    )(gate, mix, inp, taps, q, k, v, lam, gain.reshape(1, -1), wc, wh)


def solution(mesh):
    placed = (
        P("sp", "tp"),
        P("sp", "tp"),
        P("sp", "tp"),
        P(None, "tp"),
        P("sp", "tp"),
        P("sp", "tp"),
        P("sp", "tp"),
        P("tp"),
        P(),
        P("tp", None),
        P("tp", None),
    )
    return jax.shard_map(
        functools.partial(shards, mesh.shape["sp"], mesh.shape["tp"]),
        mesh=mesh,
        in_specs=placed,
        out_specs=P(("sp", "tp"), None),
        check_vma=False,
    )
```
